32 devices in a mesh: kv: 8 (over z, y), tp: 4 (over x, core).
Axes of the slice: x: 2, y: 2, z: 4, core: 2. Of those that a mesh axis runs over, the one named last changes fastest.
Arguments:
- tokens: bfloat16 [32, 6, 2048], replicated, may hold values from -6 to 6
- in_gain: bfloat16 [2048], replicated, may hold values from 0.099609375 to 1.8984375
- w_down_q: bfloat16 [2048, 512], P('kv'), may hold values from -0.125 to 0.125
- w_down_kv: bfloat16 [2048, 256], P('kv'), may hold values from -0.125 to 0.125
- w_rope_key: bfloat16 [2048, 32], replicated, may hold values from -0.125 to 0.125
- q_gain: bfloat16 [512], replicated, may hold values from 0.099609375 to 1.8984375
- kv_gain: bfloat16 [256], replicated, may hold values from 0.099609375 to 1.8984375
- w_up_q: bfloat16 [512, 1536], P(None, 'tp'), may hold values from -0.25 to 0.25
- w_absorb: bfloat16 [16, 64, 256], P('tp'), may hold values from -0.75 to 0.75
- w_value: bfloat16 [256, 1024], P(None, 'tp'), may hold values from -0.375 to 0.375
- w_out: bfloat16 [1024, 2048], P('tp'), may hold values from -0.1875 to 0.1875
- out_gain: bfloat16 [2048], replicated, may hold values from 0.099609375 to 1.8984375
- cache: bfloat16 [32, 16384, 288], P(None, 'kv'), may hold values from -1300 to 1300
- cached: int32 [32], replicated, may hold values from 1 to 16372, as said below
- accepted: int32 [32], replicated, may hold values from 0 to 6
- parents: int32 [32, 6], replicated, may hold values from -1 to 4, as said below
Outputs:
- attended: bfloat16 [32, 6, 2048], P('tp')
- new_cache: bfloat16 [32, 16384, 288], P(None, 'kv')
The draws below stay inside these ranges and needn't reach their ends.
Inputs may be any that keep to these rules, and one draw needn't show every extreme that they name: Some sequence has at least 15360 cached positions and some has at most 12. parents[s, j] is -1 or less than j.
All inputs are finite; a program needn't handle non-finite values.
Results may differ from the reference program's by a relative error of at most 0.023.
The reference program's roundings to bfloat16 on the way (of `normed`, `query_in`, `latent`, `rope_key`, `query_lat`, `lat_out` and `head_out`) count: a program that leaves them out, or rounds other values in their place, can miss the bound.
Values may be sent and summed in bfloat16 or wider, within the bound.
A program may use at most 320 MiB of HBM per device.

```python
import jax
import jax.numpy as jnp
from jax import lax

D = 2048
Q_RANK = 512
KV_RANK = 256
HEADS = 16
NOPE = 64
ROPE = 32
VDIM = 64
PROP = 6
SEQS = 32
CTX_DEV = 2048
CTX = 16384
N_KV = 8
N_TP = 4


def shared_lengths(key):
    top_len = CTX - 2 * PROP
    powers = jax.random.randint(jax.random.fold_in(key, 21), (SEQS,), 1, top_len.bit_length() + 1)
    ceiling = jnp.minimum(jnp.left_shift(jnp.ones((SEQS,), jnp.int32), powers), top_len)
    lengths = jax.random.randint(jax.random.fold_in(key, 22), (SEQS,), 1, ceiling + 1)
    ordering = jax.random.permutation(jax.random.fold_in(key, 23), SEQS)
    longest = jax.random.randint(jax.random.fold_in(key, 24), (), CTX - CTX_DEV // 2, top_len + 1)
    shortest = jax.random.randint(jax.random.fold_in(key, 25), (), 1, 2 * PROP + 1)
    lengths = lengths.at[ordering[0]].set(longest)
    lengths = lengths.at[ordering[1]].set(shortest)
    return lengths.astype(jnp.int32)


def draw_cache(key, part):
    sample = jnp.clip(jax.random.normal(jax.random.fold_in(key, 11), (SEQS, CTX, KV_RANK + ROPE), jnp.float32), -6.0, 6.0)
    lengths = shared_lengths(key)
    places = jnp.arange(CTX, dtype=jnp.int32)[None, :]
    recent = (places < lengths[:, None]) & (places >= lengths[:, None] - CTX_DEV // 4)
    boost = jnp.where(recent, 3.0, 1.0)[:, :, None]
    latent = sample[:, :, :KV_RANK] * boost
    sample = jnp.concatenate([latent, sample[:, :, KV_RANK:]], axis=-1)
    return sample.astype(jnp.bfloat16)


def draw_cached(key, part):
    return shared_lengths(key)


def draw_parents(key, part):
    limits = jnp.arange(1, PROP + 1, dtype=jnp.int32)
    picks = jax.random.randint(jax.random.fold_in(key, 31), (SEQS, PROP), 0, limits)
    parents = (picks - 1).astype(jnp.int32)
    deepest = jax.random.randint(jax.random.fold_in(key, 32), (), 0, SEQS)
    parents = parents.at[deepest, PROP - 1].set(PROP - 2)
    return parents.astype(jnp.int32)


def touch_ends(values, own_key, low, high):
    extent = values.shape
    place = [jax.random.randint(jax.random.fold_in(own_key, axis), (), 0, extent[axis]) for axis in range(len(extent))]
    values = values.at[tuple(place)].set(low)
    longest = extent.index(max(extent))
    place[longest] = (place[longest] + 1) % extent[longest]
    return values.at[tuple(place)].set(high)


def shard_levels(key, dims, split, least, high):
    level, own = 1.0, jax.random.fold_in(key, 6)
    for position, shards_of in split:
        heights = jnp.exp(jax.random.uniform(jax.random.fold_in(own, position), (shards_of,), jnp.float32, least / len(split), high / len(split)))
        level = level * jnp.repeat(heights, dims[position] // shards_of).reshape([-1 if axis == position else 1 for axis in range(len(dims))])
    return level


def centred(rng, shape, deviation, limit, split=(), kind=jnp.bfloat16):
    result = jax.random.normal(rng, shape, jnp.float32) * deviation
    if len(split) > 0:
        result = shard_levels(rng, shape, split, -0.22, 0.18) * result
    return jnp.clip(result, min=-limit, max=limit).astype(kind)


def setup_inputs(seed: int = 0) -> dict:
    keys = jax.random.split(jax.random.key(seed), 17)
    tokens = centred(keys[0], (SEQS, PROP, D), 1.0, 6.0)
    in_gain = jnp.clip(1.0 + 0.18 * jax.random.normal(keys[1], (D,), jnp.float32), 0.099609375, 1.8984375).astype(jnp.bfloat16)
    w_down_q = centred(keys[2], (D, Q_RANK), D ** -0.5, 0.125, ((0, 8),))
    w_down_kv = centred(keys[3], (D, KV_RANK), D ** -0.5, 0.125, ((0, 8),))
    w_rope_key = centred(keys[4], (D, ROPE), D ** -0.5, 0.125)
    q_gain = jnp.clip(1.0 + 0.18 * jax.random.normal(keys[5], (Q_RANK,), jnp.float32), 0.099609375, 1.8984375).astype(jnp.bfloat16)
    kv_gain = jnp.clip(1.0 + 0.18 * jax.random.normal(keys[6], (KV_RANK,), jnp.float32), 0.099609375, 1.8984375).astype(jnp.bfloat16)
    w_up_q = centred(keys[7], (Q_RANK, HEADS * (NOPE + ROPE)), Q_RANK ** -0.5, 0.25, ((1, 4),))
    w_absorb = centred(keys[8], (HEADS, NOPE, KV_RANK), NOPE ** -0.5, 0.75, ((0, 4),))
    w_value = centred(keys[9], (KV_RANK, HEADS * VDIM), KV_RANK ** -0.5, 0.375, ((1, 4),))
    w_out = centred(keys[10], (HEADS * VDIM, D), (HEADS * VDIM) ** -0.5, 0.1875, ((0, 4),))
    out_gain = jnp.clip(1.0 + 0.18 * jax.random.normal(keys[11], (D,), jnp.float32), 0.099609375, 1.8984375).astype(jnp.bfloat16)
    cache = draw_cache(jax.random.fold_in(keys[16], 71), 0)
    cached = draw_cached(jax.random.fold_in(keys[16], 71), 0)
    accepted = touch_ends(jax.random.randint(keys[14], (SEQS,), 0, PROP + 1), jax.random.fold_in(keys[14], 1), 0, PROP).astype(jnp.int32)
    parents = draw_parents(jax.random.fold_in(keys[16], 71), 0)
    return dict(tokens=tokens, in_gain=in_gain, w_down_q=w_down_q, w_down_kv=w_down_kv, w_rope_key=w_rope_key, q_gain=q_gain, kv_gain=kv_gain, w_up_q=w_up_q, w_absorb=w_absorb, w_value=w_value, w_out=w_out, out_gain=out_gain, cache=cache, cached=cached, accepted=accepted, parents=parents)


EPSILON = 1e-06
ROTARY_BASE = 10000.0
FLOOR_SCORE = -1e+30

def round_trip(values):
    return lax.optimization_barrier(values.astype(jnp.bfloat16)).astype(jnp.float32)

def rms_scale(values, gain_vec):
    floats = values.astype(jnp.float32)
    return floats * lax.rsqrt(lax.optimization_barrier(jnp.mean(floats * floats, axis=-1, keepdims=True)) + EPSILON) * gain_vec.astype(jnp.float32)

def rotate(values, positions):
    half_width = values.shape[-1] // 2
    frequency = ROTARY_BASE ** (-jnp.arange(half_width, dtype=jnp.float32) * 2.0 / values.shape[-1])
    angles = positions.astype(jnp.float32)[..., None] * frequency
    cosine = jnp.cos(angles)
    sine_part = jnp.sin(angles)
    lower_half = values[..., :half_width]
    upper_half = values[..., half_width:]
    return jnp.concatenate([lower_half * cosine - upper_half * sine_part, lower_half * sine_part + upper_half * cosine], axis=-1)

def ancestry(parents):
    num_prop = parents.shape[-1]
    slot_ids = jnp.arange(num_prop, dtype=jnp.int32)
    parent_hot = parents[:, :, None] == slot_ids[None, None, :]
    itself_mask = jnp.broadcast_to(slot_ids[:, None] == slot_ids[None, :], parent_hot.shape)
    reached = itself_mask
    for repeat in range(num_prop):
        reached = itself_mask | jnp.any(parent_hot[:, :, :, None] & reached[:, None, :, :], axis=2)
    return reached

def reference(tokens, in_gain, w_down_q, w_down_kv, w_rope_key, q_gain, kv_gain, w_up_q, w_absorb, w_value, w_out, out_gain, cache, cached, accepted, parents):
    f32 = jnp.float32
    bf16 = jnp.bfloat16
    normed = rms_scale(tokens, in_gain).astype(bf16).reshape(SEQS * PROP, D)
    query_in = rms_scale(jnp.dot(normed, w_down_q, preferred_element_type=f32), q_gain).astype(bf16)
    latent = rms_scale(jnp.dot(normed, w_down_kv, preferred_element_type=f32), kv_gain).astype(bf16)
    lengths = (cached + accepted).astype(jnp.int32)
    reached = ancestry(parents)
    depth_of = lax.optimization_barrier(jnp.sum(reached.astype(jnp.int32), axis=-1)) - 1
    positions = lengths[:, None] + depth_of
    rope_key = rotate(jnp.dot(normed, w_rope_key, preferred_element_type=f32).reshape(SEQS, PROP, ROPE), positions).astype(bf16)
    latent_rows = latent.reshape(SEQS, PROP, KV_RANK)
    new_rows = jnp.concatenate([latent_rows, rope_key], axis=-1)
    queries = jnp.dot(query_in, w_up_q, preferred_element_type=f32).reshape(SEQS, PROP, HEADS, NOPE + ROPE)
    query_nope = queries[..., :NOPE].astype(bf16)
    query_rope = rotate(queries[..., NOPE:], positions[:, :, None]).astype(bf16)
    query_lat = jnp.einsum('sphn,hnc->sphc', query_nope.astype(f32), w_absorb.astype(f32)).astype(bf16)
    score_scale = (NOPE + ROPE) ** (-0.5)
    key_pos = jnp.arange(CTX, dtype=jnp.int32)

    def one_sequence(seq_items):
        lat_q, rope_q, keys_all, length, reach_one, rows_one = seq_items
        keys_lat = keys_all[:, :KV_RANK].astype(f32)
        cache_scores = (jnp.einsum('phc,kc->phk', lat_q.astype(f32), keys_lat) + jnp.einsum('phr,kr->phk', rope_q.astype(f32), keys_all[:, KV_RANK:].astype(f32))) * score_scale
        visible = (key_pos < length).reshape(N_KV, CTX_DEV)
        blocked = cache_scores.reshape(PROP, HEADS, N_KV, CTX_DEV)
        masked = jnp.where(visible, blocked, FLOOR_SCORE)
        block_peak = lax.optimization_barrier(jnp.max(masked, axis=-1))
        weights = jnp.where(visible, jnp.exp(masked - block_peak[..., None]), 0.0)
        block_den = lax.optimization_barrier(jnp.sum(weights, axis=-1))
        block_num = jnp.einsum('phbk,bkc->phbc', round_trip(weights), keys_lat.reshape(N_KV, CTX_DEV, KV_RANK))
        rows_lat = rows_one[:, :KV_RANK].astype(f32)
        prop_scores = (jnp.einsum('phc,kc->phk', lat_q.astype(f32), rows_lat) + jnp.einsum('phr,kr->phk', rope_q.astype(f32), rows_one[:, KV_RANK:].astype(f32))) * score_scale
        allowed = reach_one[:, None, :]
        prop_masked = jnp.where(allowed, prop_scores, FLOOR_SCORE)
        prop_peak = lax.optimization_barrier(jnp.max(prop_masked, axis=-1))
        prop_weights = jnp.where(allowed, jnp.exp(prop_masked - prop_peak[..., None]), 0.0)
        prop_den = lax.optimization_barrier(jnp.sum(prop_weights, axis=-1))
        prop_num = jnp.einsum('phk,kc->phc', round_trip(prop_weights), rows_lat)
        highest = jnp.maximum(lax.optimization_barrier(jnp.max(block_peak, axis=-1)), prop_peak)
        block_factor = jnp.exp(block_peak - highest[..., None])
        prop_factor = jnp.exp(prop_peak - highest)
        numerator = lax.optimization_barrier(jnp.sum(block_num * block_factor[..., None], axis=2)) + prop_num * prop_factor[..., None]
        denominator = lax.optimization_barrier(jnp.sum(block_den * block_factor, axis=-1)) + prop_den * prop_factor
        return (numerator / denominator[..., None]).astype(bf16)
    lat_out = lax.map(one_sequence, (query_lat, query_rope, cache, lengths, reached, new_rows))
    head_out = jnp.einsum('sphc,chv->sphv', lat_out.astype(f32), w_value.reshape(KV_RANK, HEADS, VDIM).astype(f32)).astype(bf16)
    per_group = HEADS // N_TP
    grouped = head_out.reshape(SEQS * PROP, N_TP, per_group * VDIM)
    out_rows = w_out.reshape(N_TP, per_group * VDIM, D)
    partials = jnp.einsum('tgc,gcd->gtd', grouped.astype(f32), out_rows.astype(f32))
    summed = lax.optimization_barrier(jnp.sum(round_trip(partials), axis=0))
    attended = rms_scale(summed, out_gain).astype(bf16).reshape(SEQS, PROP, D)
    slot_ids = key_pos[None, :] - lengths[:, None]
    onehot = (slot_ids[:, :, None] == jnp.arange(PROP, dtype=jnp.int32)[None, None, :]).astype(f32)
    placed = jnp.einsum('skp,spc->skc', onehot, new_rows.astype(f32)).astype(bf16)
    inside = (slot_ids >= 0) & (slot_ids < PROP)
    new_cache = jnp.where(inside[:, :, None], placed, cache)
    return (attended, new_cache)
```

```python
import functools

import jax
import jax.numpy as jnp
from jax import lax
from jax.experimental import pallas as pl
from jax.experimental.pallas import tpu as pltpu
from jax.sharding import PartitionSpec as P

EPSILON = 1e-06
ROTARY_BASE = 10000.0
FLOOR_SCORE = -1e30
F32 = jnp.float32
BF16 = jnp.bfloat16


def exchange_kernel(axis, n, modes, *refs):
    count = len(modes)
    ins, outs = refs[:count], refs[count : 2 * count]
    send_sem, recv_sem, own_sem = refs[2 * count :]
    me = lax.axis_index(axis)
    barrier = pltpu.get_barrier_semaphore()
    for d in range(1, n):
        pl.semaphore_signal(
            barrier,
            inc=1,
            device_id={axis: lax.rem(me + d, n)},
            device_id_type=pl.DeviceIdType.MESH,
        )
    owns = []
    for a in range(count):
        src = ins[a] if modes[a] else ins[a].at[me]
        own = pltpu.make_async_copy(src, outs[a].at[me], own_sem.at[a])
        own.start()
        owns.append(own)
    pl.semaphore_wait(barrier, n - 1)
    copies = []
    for d in range(1, n):
        peer = lax.rem(me + d, n)
        for a in range(count):
            copy = pltpu.make_async_remote_copy(
                src_ref=ins[a] if modes[a] else ins[a].at[peer],
                dst_ref=outs[a].at[me],
                send_sem=send_sem.at[a, d],
                recv_sem=recv_sem.at[a, d],
                device_id={axis: peer},
                device_id_type=pl.DeviceIdType.MESH,
            )
            copy.start()
            copies.append(copy)
    for own in owns:
        own.wait()
    for copy in copies:
        copy.wait()


def exchange(arrays, modes, axis, n, cid):
    count = len(arrays)
    outs = [
        jax.ShapeDtypeStruct(((n,) + x.shape) if mode else x.shape, x.dtype)
        for x, mode in zip(arrays, modes)
    ]
    vmem = pl.BlockSpec(memory_space=pltpu.VMEM)
    return pl.pallas_call(
        functools.partial(exchange_kernel, axis, n, tuple(modes)),
        out_shape=outs,
        in_specs=[vmem] * count,
        out_specs=[vmem] * count,
        scratch_shapes=[
            pltpu.SemaphoreType.DMA((count, n)),
            pltpu.SemaphoreType.DMA((count, n)),
            pltpu.SemaphoreType.DMA((count,)),
        ],
        compiler_params=pltpu.CompilerParams(collective_id=cid, has_side_effects=True),
        name=f"exchange{cid}",
    )(*arrays)


def attend_kernel(ntp, nprop, latent, scale, meta, lengths, q_ref, new_ref, c_ref, o_ref, num_ref, md_ref):
    i = pl.program_id(0)
    tp = meta[0]
    offset = meta[1]
    groups = pl.num_programs(0) // ntp
    seq = lax.rem(lax.rem(i, ntp) + tp + 1, ntp) * groups + i // ntp
    span = c_ref.shape[2]
    start = lengths[seq] - offset
    o_ref[...] = c_ref[...]

    @pl.when((start > -nprop) & (start < span))
    def _():
        window = 256
        base = jnp.clip(start // 128 * 128, 0, span - window)
        base = pl.multiple_of(base, 128)
        rows = new_ref[0]
        slot = base + lax.broadcasted_iota(jnp.int32, (rows.shape[0], window), 1) - start
        which = lax.broadcasted_iota(jnp.int32, (rows.shape[0], window), 0)
        hot = ((slot == which) & (which < nprop)).astype(F32).astype(BF16)
        placed = lax.dot_general(
            rows, hot, (((0,), (0,)), ((), ())), preferred_element_type=F32
        )
        current = c_ref[0, :, pl.ds(base, window)].astype(F32)
        slot_all = base + lax.broadcasted_iota(jnp.int32, current.shape, 1) - start
        inside = (slot_all >= 0) & (slot_all < nprop)
        o_ref[0, :, pl.ds(base, window)] = jnp.where(inside, placed, current).astype(BF16)

    mine = lax.rem(i, ntp) == ntp - 1

    @pl.when(mine & (start > 0))
    def _():
        scores = jnp.dot(q_ref[0], c_ref[0], preferred_element_type=F32) * scale
        seen = lax.broadcasted_iota(jnp.int32, scores.shape, 1) < start
        masked = jnp.where(seen, scores, FLOOR_SCORE)
        peak = jnp.max(masked, axis=-1, keepdims=True)
        weights = jnp.where(seen, jnp.exp(masked - peak), 0.0)
        den = jnp.sum(weights, axis=-1, keepdims=True)
        num = lax.dot_general(
            weights.astype(BF16),
            c_ref[0, :latent, :],
            (((1,), (1,)), ((), ())),
            preferred_element_type=F32,
        )
        num_ref[0] = num.astype(BF16)
        lane = lax.broadcasted_iota(jnp.int32, (scores.shape[0], 128), 1)
        both = jnp.where(lane == 0, peak, den)
        md_ref[0] = jnp.transpose(both)[:8]

    @pl.when(mine & (start <= 0))
    def _():
        num_ref[...] = jnp.zeros_like(num_ref)
        which = lax.broadcasted_iota(jnp.int32, md_ref.shape[1:], 0)
        md_ref[0] = jnp.where(which == 0, FLOOR_SCORE, 0.0)


def attend(cache_t, queries, new_rows, lengths, meta, ntp, nprop, latent, scale):
    seqs, width, span = cache_t.shape
    groups, rows, _ = queries.shape

    def seq_of(i, meta):
        return lax.rem(lax.rem(i, ntp) + meta[0] + 1, ntp) * groups + i // ntp

    return pl.pallas_call(
        functools.partial(attend_kernel, ntp, nprop, latent, scale),
        grid_spec=pltpu.PrefetchScalarGridSpec(
            num_scalar_prefetch=2,
            grid=(seqs,),
            in_specs=[
                pl.BlockSpec((1, rows, width), lambda i, meta, lengths: (i // ntp, 0, 0)),
                pl.BlockSpec(
                    (1,) + new_rows.shape[1:], lambda i, meta, lengths: (seq_of(i, meta), 0, 0)
                ),
                pl.BlockSpec((1, width, span), lambda i, meta, lengths: (seq_of(i, meta), 0, 0)),
            ],
            out_specs=[
                pl.BlockSpec((1, width, span), lambda i, meta, lengths: (seq_of(i, meta), 0, 0)),
                pl.BlockSpec((1, rows, latent), lambda i, meta, lengths: (i // ntp, 0, 0)),
                pl.BlockSpec((1, 8, rows), lambda i, meta, lengths: (i // ntp, 0, 0)),
            ],
        ),
        out_shape=[
            jax.ShapeDtypeStruct(cache_t.shape, cache_t.dtype),
            jax.ShapeDtypeStruct((groups, rows, latent), BF16),
            jax.ShapeDtypeStruct((groups, 8, rows), F32),
        ],
        compiler_params=pltpu.CompilerParams(dimension_semantics=("arbitrary",)),
        name="attend",
    )(meta, lengths, queries, new_rows, cache_t)


def rms_scale(values, gain_vec):
    floats = values.astype(F32)
    return (
        floats
        * lax.rsqrt(jnp.mean(floats * floats, axis=-1, keepdims=True) + EPSILON)
        * gain_vec.astype(F32)
    )


def rotate(values, cosine, sine):
    half = values.shape[-1] // 2
    low, high = values[..., :half], values[..., half:]
    return jnp.concatenate([low * cosine - high * sine, low * sine + high * cosine], axis=-1)


def ancestor_bits(parents):
    masks = []
    for j in range(parents.shape[-1]):
        mask = jnp.full(parents.shape[:1], 1 << j, jnp.int32)
        for k in range(j):
            mask = mask | jnp.where(parents[:, j] == k, masks[k], 0)
        masks.append(mask)
    return jnp.stack(masks, axis=-1)


def pad_front(x, size):
    if x.shape[0] == size:
        return x
    return jnp.pad(x, [(0, size - x.shape[0])] + [(0, 0)] * (x.ndim - 1))


def local(
    nkv, ntp, tokens, in_gain, w_down_q, w_down_kv, w_rope_key, q_gain, kv_gain, w_up_q,
    w_absorb, w_value, w_out, out_gain, cache, cached, accepted, parents,
):
    seqs, nprop, model = tokens.shape
    down = w_down_q.shape[0]
    q_rank = w_down_q.shape[1]
    latent_w = w_down_kv.shape[1]
    rope_w = w_rope_key.shape[1]
    heads, nope = w_absorb.shape[:2]
    value_w = w_value.shape[1] // heads
    span = cache.shape[1]
    per_tp = seqs // ntp
    kv = lax.axis_index("kv")
    tp = lax.axis_index("tp")
    slot = jnp.minimum(kv, per_tp - 1)
    scale = (nope + rope_w) ** (-0.5)

    normed = rms_scale(tokens, in_gain).astype(BF16)
    own_seqs = lax.dynamic_slice_in_dim(normed, tp * per_tp, per_tp, 0)
    own_cols = lax.dynamic_slice_in_dim(own_seqs, kv * down, down, 2)
    w_down = jnp.concatenate([w_down_q, w_down_kv], axis=1)
    partial = jnp.dot(own_cols, w_down, preferred_element_type=F32)
    (parts,) = exchange([pad_front(partial, nkv)], [False], "kv", nkv, 1)
    sums = jnp.sum(parts, axis=0)
    query_in = rms_scale(sums[:, :q_rank], q_gain).astype(BF16)
    latent = rms_scale(sums[:, q_rank:], kv_gain).astype(BF16)
    query_in, latents = exchange([query_in, latent], [True, True], "tp", ntp, 2)

    lengths = cached + accepted
    bits = ancestor_bits(parents)
    positions = lengths[:, None] + lax.population_count(bits) - 1
    half = rope_w // 2
    frequency = ROTARY_BASE ** (-jnp.arange(half, dtype=F32) * 2.0 / rope_w)
    angles = positions.astype(F32)[..., None] * frequency
    cosine, sine = jnp.cos(angles), jnp.sin(angles)
    rope_key = rotate(
        jnp.dot(normed, w_rope_key, preferred_element_type=F32), cosine, sine
    ).astype(BF16)

    cos_own = lax.dynamic_index_in_dim(cosine.reshape(ntp, per_tp, nprop, half), slot, 1, False)
    sin_own = lax.dynamic_index_in_dim(sine.reshape(ntp, per_tp, nprop, half), slot, 1, False)
    queries = jnp.dot(query_in, w_up_q, preferred_element_type=F32).reshape(
        ntp, nprop, heads, nope + rope_w
    )
    query_rope = rotate(
        queries[..., nope:], cos_own[:, :, None], sin_own[:, :, None]
    ).astype(BF16)
    query_lat = jnp.einsum(
        "sphn,hnc->sphc", queries[..., :nope].astype(BF16), w_absorb, preferred_element_type=F32
    ).astype(BF16)
    full = jnp.concatenate([query_lat, query_rope], axis=-1).reshape(ntp, nprop * heads, -1)
    (full,) = exchange([full], [False], "tp", ntp, 3)
    rows = ntp * nprop * heads
    full = full.reshape(rows, latent_w + rope_w)
    all_queries, all_latents = exchange([full, latents], [True, True], "kv", nkv, 4)

    new_latents = all_latents[:per_tp].transpose(1, 0, 2, 3).reshape(seqs, nprop, latent_w)
    new_rows = jnp.concatenate([new_latents, rope_key], axis=-1)
    padded = jnp.pad(new_rows, ((0, 0), (0, -nprop % 16), (0, 0)))
    meta = jnp.stack([tp, kv * span]).astype(jnp.int32)
    cache_t, num, md = attend(
        cache.transpose(0, 2, 1), all_queries[:per_tp], padded, lengths, meta, ntp, nprop,
        latent_w, scale,
    )
    num, md = exchange(
        [pad_front(num, nkv), pad_front(md, nkv)], [False, False], "kv", nkv, 5
    )

    mine = tp * per_tp + slot
    my_rows = lax.dynamic_index_in_dim(new_rows, mine, 0, False)
    my_bits = lax.dynamic_index_in_dim(bits, mine, 0, False)
    row_prop = jnp.arange(rows) // heads % nprop
    row_bits = jnp.sum(
        jnp.where(row_prop[:, None] == jnp.arange(nprop)[None, :], my_bits[None, :], 0), axis=-1
    )
    allowed = ((row_bits[:, None] >> jnp.arange(nprop)[None, :]) & 1) == 1
    prop_scores = jnp.einsum("rc,kc->rk", full, my_rows, preferred_element_type=F32) * scale
    prop_masked = jnp.where(allowed, prop_scores, FLOOR_SCORE)
    prop_peak = jnp.max(prop_masked, axis=-1)
    prop_weights = jnp.where(allowed, jnp.exp(prop_masked - prop_peak[:, None]), 0.0)
    prop_den = jnp.sum(prop_weights, axis=-1)
    prop_num = jnp.dot(
        prop_weights.astype(BF16), my_rows[:, :latent_w], preferred_element_type=F32
    )
    peaks, dens = md[:, 0], md[:, 1]
    top = jnp.maximum(jnp.max(peaks, axis=0), prop_peak)
    factor = jnp.exp(peaks - top[None])
    prop_factor = jnp.exp(prop_peak - top)
    total_den = jnp.sum(factor * dens, axis=0) + prop_factor * prop_den
    total_num = jnp.sum(factor[..., None] * num.astype(F32), axis=0) + (
        prop_factor[:, None] * prop_num
    )
    lat_out = (total_num / total_den[:, None]).astype(BF16)
    (lat_out,) = exchange([lat_out.reshape(ntp, nprop * heads, latent_w)], [False], "tp", ntp, 6)
    head_out = jnp.einsum(
        "sphc,chv->sphv",
        lat_out.reshape(ntp, nprop, heads, latent_w),
        w_value.reshape(latent_w, heads, value_w),
        preferred_element_type=F32,
    ).astype(BF16)
    partials = jnp.dot(
        head_out.reshape(ntp, nprop, heads * value_w), w_out, preferred_element_type=F32
    ).astype(BF16)
    (partials,) = exchange([partials], [False], "tp", ntp, 7)
    summed = jnp.sum(partials.astype(F32), axis=0)
    attended = rms_scale(summed, out_gain).astype(BF16)
    (attended,) = exchange([attended], [True], "kv", nkv, 8)
    return attended[:per_tp], cache_t.transpose(0, 2, 1)


def solution(mesh):
    placed = (
        P(), P(), P("kv", None), P("kv", None), P(), P(), P(), P(None, "tp"),
        P("tp", None, None), P(None, "tp"), P("tp", None), P(), P(None, "kv", None), P(), P(), P(),
    )
    return jax.shard_map(
        functools.partial(local, mesh.shape["kv"], mesh.shape["tp"]),
        mesh=mesh,
        in_specs=placed,
        out_specs=(P("tp", None, None), P(None, "kv", None)),
        check_vma=False,
    )
```

```python
import functools

import jax
import jax.numpy as jnp
from jax import lax
from jax.experimental import pallas as pl
from jax.experimental.pallas import tpu as pltpu
from jax.sharding import PartitionSpec as P

EPSILON = 1e-06
ROTARY_BASE = 10000.0
FLOOR_SCORE = -1e30
F32 = jnp.float32
BF16 = jnp.bfloat16


def exchange_kernel(axis, n, modes, *refs):
    count = len(modes)
    ins, outs = refs[:count], refs[count : 2 * count]
    send_sem, recv_sem, own_sem = refs[2 * count :]
    me = lax.axis_index(axis)
    barrier = pltpu.get_barrier_semaphore()
    for d in range(1, n):
        pl.semaphore_signal(
            barrier,
            inc=1,
            device_id={axis: lax.rem(me + d, n)},
            device_id_type=pl.DeviceIdType.MESH,
        )
    owns = []
    for a in range(count):
        src = ins[a] if modes[a] else ins[a].at[me]
        own = pltpu.make_async_copy(src, outs[a].at[me], own_sem.at[a])
        own.start()
        owns.append(own)
    pl.semaphore_wait(barrier, n - 1)
    copies = []
    for d in range(1, n):
        peer = lax.rem(me + d, n)
        for a in range(count):
            copy = pltpu.make_async_remote_copy(
                src_ref=ins[a] if modes[a] else ins[a].at[peer],
                dst_ref=outs[a].at[me],
                send_sem=send_sem.at[a, d],
                recv_sem=recv_sem.at[a, d],
                device_id={axis: peer},
                device_id_type=pl.DeviceIdType.MESH,
            )
            copy.start()
            copies.append(copy)
    for own in owns:
        own.wait()
    for copy in copies:
        copy.wait()


def exchange(arrays, modes, axis, n, cid):
    count = len(arrays)
    outs = [
        jax.ShapeDtypeStruct(((n,) + x.shape) if mode else x.shape, x.dtype)
        for x, mode in zip(arrays, modes)
    ]
    vmem = pl.BlockSpec(memory_space=pltpu.VMEM)
    return pl.pallas_call(
        functools.partial(exchange_kernel, axis, n, tuple(modes)),
        out_shape=outs,
        in_specs=[vmem] * count,
        out_specs=[vmem] * count,
        scratch_shapes=[
            pltpu.SemaphoreType.DMA((count, n)),
            pltpu.SemaphoreType.DMA((count, n)),
            pltpu.SemaphoreType.DMA((count,)),
        ],
        compiler_params=pltpu.CompilerParams(collective_id=cid, has_side_effects=True),
        name=f"exchange{cid}",
    )(*arrays)


def attend_kernel(ntp, nprop, latent, scale, meta, lengths, q_ref, new_ref, c_ref, o_ref, num_ref, md_ref):
    i = pl.program_id(0)
    tp = meta[0]
    offset = meta[1]
    groups = pl.num_programs(0)
    span = c_ref.shape[3]
    o_ref[...] = c_ref[...]

    for g in range(ntp):
        begin = lengths[g * groups + i] - offset

        @pl.when((begin > -nprop) & (begin < span))
        def _(g=g, begin=begin):
            window = 256
            base = jnp.clip(begin // 128 * 128, 0, span - window)
            base = pl.multiple_of(base, 128)
            rows = new_ref[g, 0]
            slot = base + lax.broadcasted_iota(jnp.int32, (rows.shape[0], window), 1) - begin
            which = lax.broadcasted_iota(jnp.int32, (rows.shape[0], window), 0)
            hot = ((slot == which) & (which < nprop)).astype(F32).astype(BF16)
            placed = lax.dot_general(
                rows, hot, (((0,), (0,)), ((), ())), preferred_element_type=F32
            )
            current = c_ref[g, 0, :, pl.ds(base, window)].astype(F32)
            slot_all = base + lax.broadcasted_iota(jnp.int32, current.shape, 1) - begin
            inside = (slot_all >= 0) & (slot_all < nprop)
            o_ref[g, 0, :, pl.ds(base, window)] = jnp.where(inside, placed, current).astype(BF16)

    start = lengths[tp * groups + i] - offset

    @pl.when(start > 0)
    def _():
        scores = jnp.dot(q_ref[0], c_ref[tp, 0], preferred_element_type=F32) * scale
        seen = lax.broadcasted_iota(jnp.int32, scores.shape, 1) < start
        masked = jnp.where(seen, scores, FLOOR_SCORE)
        peak = jnp.max(masked, axis=-1, keepdims=True)
        weights = jnp.where(seen, jnp.exp(masked - peak), 0.0)
        den = jnp.sum(weights, axis=-1, keepdims=True)
        num = lax.dot_general(
            weights.astype(BF16),
            c_ref[tp, 0, :latent, :],
            (((1,), (1,)), ((), ())),
            preferred_element_type=F32,
        )
        num_ref[0] = num.astype(BF16)
        lane = lax.broadcasted_iota(jnp.int32, (scores.shape[0], 128), 1)
        both = jnp.where(lane == 0, peak, den)
        md_ref[0] = jnp.transpose(both)[:8]

    @pl.when(start <= 0)
    def _():
        num_ref[...] = jnp.zeros_like(num_ref)
        which = lax.broadcasted_iota(jnp.int32, md_ref.shape[1:], 0)
        md_ref[0] = jnp.where(which == 0, FLOOR_SCORE, 0.0)


def attend(cache_t, queries, new_rows, lengths, meta, ntp, nprop, latent, scale):
    seqs, width, span = cache_t.shape
    groups, rows, _ = queries.shape
    cache_g = cache_t.reshape(ntp, groups, width, span)
    new_g = new_rows.reshape((ntp, groups) + new_rows.shape[1:])
    return pl.pallas_call(
        functools.partial(attend_kernel, ntp, nprop, latent, scale),
        grid_spec=pltpu.PrefetchScalarGridSpec(
            num_scalar_prefetch=2,
            grid=(groups,),
            in_specs=[
                pl.BlockSpec((1, rows, width), lambda i, meta, lengths: (i, 0, 0)),
                pl.BlockSpec(
                    (ntp, 1) + new_g.shape[2:], lambda i, meta, lengths: (0, i, 0, 0)
                ),
                pl.BlockSpec((ntp, 1, width, span), lambda i, meta, lengths: (0, i, 0, 0)),
            ],
            out_specs=[
                pl.BlockSpec((ntp, 1, width, span), lambda i, meta, lengths: (0, i, 0, 0)),
                pl.BlockSpec((1, rows, latent), lambda i, meta, lengths: (i, 0, 0)),
                pl.BlockSpec((1, 8, rows), lambda i, meta, lengths: (i, 0, 0)),
            ],
        ),
        out_shape=[
            jax.ShapeDtypeStruct(cache_g.shape, cache_t.dtype),
            jax.ShapeDtypeStruct((groups, rows, latent), BF16),
            jax.ShapeDtypeStruct((groups, 8, rows), F32),
        ],
        compiler_params=pltpu.CompilerParams(dimension_semantics=("arbitrary",)),
        name="attend",
    )(meta, lengths, queries, new_g, cache_g)


def rms_scale(values, gain_vec):
    floats = values.astype(F32)
    return (
        floats
        * lax.rsqrt(jnp.mean(floats * floats, axis=-1, keepdims=True) + EPSILON)
        * gain_vec.astype(F32)
    )


def rotate(values, cosine, sine):
    half = values.shape[-1] // 2
    low, high = values[..., :half], values[..., half:]
    return jnp.concatenate([low * cosine - high * sine, low * sine + high * cosine], axis=-1)


def ancestor_bits(parents):
    masks = []
    for j in range(parents.shape[-1]):
        mask = jnp.full(parents.shape[:1], 1 << j, jnp.int32)
        for k in range(j):
            mask = mask | jnp.where(parents[:, j] == k, masks[k], 0)
        masks.append(mask)
    return jnp.stack(masks, axis=-1)


def pad_front(x, size):
    if x.shape[0] == size:
        return x
    return jnp.pad(x, [(0, size - x.shape[0])] + [(0, 0)] * (x.ndim - 1))


def local(
    nkv, ntp, tokens, in_gain, w_down_q, w_down_kv, w_rope_key, q_gain, kv_gain, w_up_q,
    w_absorb, w_value, w_out, out_gain, cache, cached, accepted, parents,
):
    seqs, nprop, model = tokens.shape
    down = w_down_q.shape[0]
    q_rank = w_down_q.shape[1]
    latent_w = w_down_kv.shape[1]
    rope_w = w_rope_key.shape[1]
    heads, nope = w_absorb.shape[:2]
    value_w = w_value.shape[1] // heads
    span = cache.shape[1]
    per_tp = seqs // ntp
    kv = lax.axis_index("kv")
    tp = lax.axis_index("tp")
    slot = jnp.minimum(kv, per_tp - 1)
    scale = (nope + rope_w) ** (-0.5)

    normed = rms_scale(tokens, in_gain).astype(BF16)
    own_seqs = lax.dynamic_slice_in_dim(normed, tp * per_tp, per_tp, 0)
    own_cols = lax.dynamic_slice_in_dim(own_seqs, kv * down, down, 2)
    w_down = jnp.concatenate([w_down_q, w_down_kv], axis=1)
    partial = jnp.dot(own_cols, w_down, preferred_element_type=F32)
    (parts,) = exchange([pad_front(partial, nkv)], [False], "kv", nkv, 1)
    sums = jnp.sum(parts, axis=0)
    query_in = rms_scale(sums[:, :q_rank], q_gain).astype(BF16)
    latent = rms_scale(sums[:, q_rank:], kv_gain).astype(BF16)
    query_in, latents = exchange([query_in, latent], [True, True], "tp", ntp, 2)

    lengths = cached + accepted
    bits = ancestor_bits(parents)
    positions = lengths[:, None] + lax.population_count(bits) - 1
    half = rope_w // 2
    frequency = ROTARY_BASE ** (-jnp.arange(half, dtype=F32) * 2.0 / rope_w)
    angles = positions.astype(F32)[..., None] * frequency
    cosine, sine = jnp.cos(angles), jnp.sin(angles)
    rope_key = rotate(
        jnp.dot(normed, w_rope_key, preferred_element_type=F32), cosine, sine
    ).astype(BF16)

    cos_own = lax.dynamic_index_in_dim(cosine.reshape(ntp, per_tp, nprop, half), slot, 1, False)
    sin_own = lax.dynamic_index_in_dim(sine.reshape(ntp, per_tp, nprop, half), slot, 1, False)
    queries = jnp.dot(query_in, w_up_q, preferred_element_type=F32).reshape(
        ntp, nprop, heads, nope + rope_w
    )
    query_rope = rotate(
        queries[..., nope:], cos_own[:, :, None], sin_own[:, :, None]
    ).astype(BF16)
    query_lat = jnp.einsum(
        "sphn,hnc->sphc", queries[..., :nope].astype(BF16), w_absorb, preferred_element_type=F32
    ).astype(BF16)
    full = jnp.concatenate([query_lat, query_rope], axis=-1).reshape(ntp, nprop * heads, -1)
    (full,) = exchange([full], [False], "tp", ntp, 3)
    rows = ntp * nprop * heads
    full = full.reshape(rows, latent_w + rope_w)
    all_queries, all_latents = exchange([full, latents], [True, True], "kv", nkv, 4)

    new_latents = all_latents[:per_tp].transpose(1, 0, 2, 3).reshape(seqs, nprop, latent_w)
    new_rows = jnp.concatenate([new_latents, rope_key], axis=-1)
    padded = jnp.pad(new_rows, ((0, 0), (0, -nprop % 16), (0, 0)))
    meta = jnp.stack([tp, kv * span]).astype(jnp.int32)
    cache_t, num, md = attend(
        cache.transpose(0, 2, 1), all_queries[:per_tp], padded, lengths, meta, ntp, nprop,
        latent_w, scale,
    )
    num, md = exchange(
        [pad_front(num, nkv), pad_front(md, nkv)], [False, False], "kv", nkv, 5
    )

    mine = tp * per_tp + slot
    my_rows = lax.dynamic_index_in_dim(new_rows, mine, 0, False)
    my_bits = lax.dynamic_index_in_dim(bits, mine, 0, False)
    row_prop = jnp.arange(rows) // heads % nprop
    row_bits = jnp.sum(
        jnp.where(row_prop[:, None] == jnp.arange(nprop)[None, :], my_bits[None, :], 0), axis=-1
    )
    allowed = ((row_bits[:, None] >> jnp.arange(nprop)[None, :]) & 1) == 1
    prop_scores = jnp.einsum("rc,kc->rk", full, my_rows, preferred_element_type=F32) * scale
    prop_masked = jnp.where(allowed, prop_scores, FLOOR_SCORE)
    prop_peak = jnp.max(prop_masked, axis=-1)
    prop_weights = jnp.where(allowed, jnp.exp(prop_masked - prop_peak[:, None]), 0.0)
    prop_den = jnp.sum(prop_weights, axis=-1)
    prop_num = jnp.dot(
        prop_weights.astype(BF16), my_rows[:, :latent_w], preferred_element_type=F32
    )
    peaks, dens = md[:, 0], md[:, 1]
    top = jnp.maximum(jnp.max(peaks, axis=0), prop_peak)
    factor = jnp.exp(peaks - top[None])
    prop_factor = jnp.exp(prop_peak - top)
    total_den = jnp.sum(factor * dens, axis=0) + prop_factor * prop_den
    total_num = jnp.sum(factor[..., None] * num.astype(F32), axis=0) + (
        prop_factor[:, None] * prop_num
    )
    lat_out = (total_num / total_den[:, None]).astype(BF16)
    (lat_out,) = exchange([lat_out.reshape(ntp, nprop * heads, latent_w)], [False], "tp", ntp, 6)
    head_out = jnp.einsum(
        "sphc,chv->sphv",
        lat_out.reshape(ntp, nprop, heads, latent_w),
        w_value.reshape(latent_w, heads, value_w),
        preferred_element_type=F32,
    ).astype(BF16)
    partials = jnp.dot(
        head_out.reshape(ntp, nprop, heads * value_w), w_out, preferred_element_type=F32
    ).astype(BF16)
    (partials,) = exchange([partials], [False], "tp", ntp, 7)
    summed = jnp.sum(partials.astype(F32), axis=0)
    attended = rms_scale(summed, out_gain).astype(BF16)
    (attended,) = exchange([attended], [True], "kv", nkv, 8)
    return attended[:per_tp], cache_t.reshape(seqs, -1, span).transpose(0, 2, 1)


def solution(mesh):
    placed = (
        P(), P(), P("kv", None), P("kv", None), P(), P(), P(), P(None, "tp"),
        P("tp", None, None), P(None, "tp"), P("tp", None), P(), P(None, "kv", None), P(), P(), P(),
    )
    return jax.shard_map(
        functools.partial(local, mesh.shape["kv"], mesh.shape["tp"]),
        mesh=mesh,
        in_specs=placed,
        out_specs=(P("tp", None, None), P(None, "kv", None)),
        check_vma=False,
    )
```
